32 devices in a mesh: grp: 2 (over x), ep: 8 (over z, y), tp: 2 (over core).
Axes of the slice: x: 2, y: 2, z: 4, core: 2. Of those that a mesh axis runs over, the one named last changes fastest.
Arguments:
- tokens: bfloat16 [8192, 2048], P(('grp', 'ep'), 'tp'), parts along dimension 0, may hold values from -6 to 6
- norm_gain: float32 [2048], replicated, may hold values from 0.1 to 1.9
- expert_ids: int32 [8192, 2], P(('grp', 'ep')), parts along dimension 0, may hold values from 0 to 7, all different within a row; in each aligned block of 512 rows (0 to 511, 512 to 1023, ...) at most 192 rows name the same one
- route_weights: float32 [8192, 2], P(('grp', 'ep')), parts along dimension 0, may hold values from 0.1 to 1
- gate_weight: bfloat16 [8, 2048, 512], P('ep', None, 'tp'), may hold values from -0.125 to 0.125
- up_weight: bfloat16 [8, 2048, 512], P('ep', None, 'tp'), may hold values from -0.125 to 0.125
- down_weight: bfloat16 [8, 512, 2048], P('ep', None, 'tp'), may hold values from -0.25 to 0.25
Outputs:
- mixed: bfloat16 [8192, 2048], P(('grp', 'ep'), 'tp'), parts along dimension 0
The draws below stay inside these ranges and needn't reach their ends.
There are 2 independent parts, one for each index of `grp`. The reference program is written for one: setup_inputs(seed, part) draws one part's arguments, and reference() takes and returns one part's arrays. A program takes and returns all parts, laid end to end along the dimension named above; an argument that names none is the same for every part. Nothing has to cross between parts.
Inputs may be any that keep to these rules, and one draw needn't show every extreme that they name: `expert_ids`: each token names 2 different experts. Among the 512 tokens of one index of ep (aligned blocks of rows) at most 192 name the same expert, and in some block some expert is named by exactly 192 of them.
All inputs are finite; a program needn't handle non-finite values.
Results may differ from the reference program's by a relative error of at most 0.007.
Values may be sent and summed in bfloat16 or wider, within the bound.
A program may use at most 64 MiB of HBM per device.

```python
import math
import jax
import jax.numpy as jnp
import numpy as np
from jax import lax

D = 2048
DE = 512
TOP_K = 2
TOK_DEV = 512
EXPERTS = 8
TOKENS = 4096
CAP = 192
N_EP = 8


def levels(key, dims, pieces, least, high):
    def one(dim, parts):
        draws = jax.random.uniform(jax.random.fold_in(jax.random.fold_in(key, 6), dim), (parts,), jnp.float32, least / len(pieces), high / len(pieces))
        return jnp.repeat(jnp.exp(draws), dims[dim] // parts).reshape((-1,) + (1,) * (len(dims) - dim - 1))

    factor_of = one(*pieces[0])
    for cut in pieces[1:]:
        factor_of = factor_of * one(*cut)
    return factor_of


def shared_out(own_key, own, number, rows, amount, top, bound, lean):
    sequence = jax.random.permutation(own_key, amount)
    crowded, ordinary = shares(amount, rows * top, bound, lean, True), shares(amount, rows * top, bound, lean, False)
    places = jnp.arange(amount)

    def named(lengths, turn):
        used = int((lengths > 0).sum())
        fixed = max(1, used // 4)
        passed = fixed + (places - fixed + turn * (used - fixed)) % max(1, amount - fixed)
        return jnp.zeros((amount,), jnp.int32).at[sequence[jnp.where(places < fixed, places, passed)]].set(jnp.asarray(lengths, jnp.int32))

    lengths = jnp.where(number % 4 == 0, named(crowded, number // 4), named(ordinary, number - number // 4 - 1))
    mixed = jax.random.permutation(jax.random.fold_in(own, 3), amount)
    giver, receiver = mixed[0:amount // 2 * 2:2], mixed[1:amount // 2 * 2:2]
    room = jnp.minimum(lengths[giver] - 1, bound - lengths[receiver]) // 2
    room = jnp.where((giver == sequence[0]) | (receiver == sequence[0]) | (lengths[receiver] == 0), 0, jnp.maximum(room, 0))
    passed = jax.random.randint(jax.random.fold_in(own, 4), (amount // 2,), 0, 1 << 20) % (room + 1)
    lengths = lengths.at[giver].add(-passed).at[receiver].add(passed)
    labels = jnp.searchsorted(jnp.cumsum(lengths), jnp.arange(rows * top), side="right").astype(jnp.int32)
    table = labels.reshape(top, rows).T
    table = table[jax.random.permutation(jax.random.fold_in(own, 1), rows)]
    turn = jax.random.randint(jax.random.fold_in(own, 2), (rows, 1), 0, top)
    return jnp.take_along_axis(table, (jnp.arange(top)[None, :] + turn) % top, axis=1)


def shares(amount, total, bound, lean, full):
    portions = [(1 << 20) // math.isqrt(grade ** lean) + 1 for grade in range(1, amount + 1)]
    largest = bound if full else min(bound, max(-(-total // amount), total * portions[0] // sum(portions)))
    least = 1 if total - largest >= amount - 1 else 0
    counts, surplus = [largest] + [least] * (amount - 1), total - largest - least * (amount - 1)
    while surplus > 0:
        free = [i for i in range(1, amount) if counts[i] < largest] or [i for i in range(1, amount) if counts[i] < bound]
        whole, remaining = sum([portions[i] for i in free]), surplus
        for i in free:
            extra = min(bound - counts[i], max(1, remaining * portions[i] // whole), surplus)
            counts[i] = counts[i] + extra
            surplus = surplus - extra
    return np.array(counts)


def gaussian(own_key, extent, scale, limit, split=(), kind=jnp.bfloat16):
    entries = scale * jax.random.normal(own_key, extent, jnp.float32)
    if split:
        entries = entries * levels(own_key, extent, split, -0.22, 0.18)
    return jnp.clip(entries, -limit, limit).astype(kind)


def setup_inputs(seed: int = 0, part: int = 0) -> dict:
    key_of = jax.random.split(jax.random.key(seed), 8)
    own_keys = jax.random.split(jax.random.fold_in(key_of[7], part), 8)
    tokens = gaussian(own_keys[0], (TOKENS, D), 1.0, 6.0, ((0, 8), (1, 2)))
    norm_gain = jnp.clip(1.0 + 0.18 * jax.random.normal(key_of[1], (D,), jnp.float32), 0.1, 1.9)
    expert_ids_keys = jax.random.split(jax.random.fold_in(own_keys[2], 1), TOKENS // TOK_DEV)
    expert_ids_turns = jax.random.permutation(jax.random.fold_in(own_keys[2], 3), TOKENS // TOK_DEV)
    expert_ids = jax.vmap(lambda own, number: shared_out(jax.random.fold_in(own_keys[2], 2), own, number, TOK_DEV, EXPERTS, TOP_K, CAP, 2))(expert_ids_keys, expert_ids_turns).reshape((TOKENS, TOP_K))
    route_weights = jnp.clip(jnp.exp(math.log(1.0) - 2.3025851 * jax.random.uniform(own_keys[3], (TOKENS, TOP_K), jnp.float32) ** levels(own_keys[3], (TOKENS, TOP_K), ((0, 8),), -0.2, 0.2)), 0.1, 1.0)
    gate_weight = gaussian(key_of[4], (EXPERTS, D, DE), D ** -0.5, 0.125, ((0, 8), (2, 2)))
    up_weight = gaussian(key_of[5], (EXPERTS, D, DE), D ** -0.5, 0.125, ((0, 8), (2, 2)))
    down_weight = gaussian(key_of[6], (EXPERTS, DE, D), DE ** -0.5, 0.25, ((0, 8), (2, 2)))
    return dict(tokens=tokens, norm_gain=norm_gain, expert_ids=expert_ids, route_weights=route_weights, gate_weight=gate_weight, up_weight=up_weight, down_weight=down_weight)


def reference(tokens, norm_gain, expert_ids, route_weights, gate_weight, up_weight, down_weight):
    xf = tokens.astype(jnp.float32)
    scale = lax.rsqrt(lax.optimization_barrier(jnp.mean(xf * xf, axis=-1, keepdims=True)) + 1e-06)
    normed = (xf * scale * norm_gain.astype(jnp.float32)[None, :]).astype(jnp.bfloat16)
    flat = expert_ids.reshape(-1).astype(jnp.int32)
    pairs = flat.shape[0]
    onehot = (flat[:, None] == jnp.arange(EXPERTS, dtype=jnp.int32)[None, :]).astype(jnp.int32)
    blocked = onehot.reshape(-1, TOK_DEV * TOP_K, EXPERTS)
    earlier = (jnp.cumsum(blocked, axis=1) - blocked).reshape(pairs, EXPERTS)
    slot = lax.optimization_barrier(jnp.sum(earlier * onehot, axis=-1)).astype(jnp.int32)
    block = (jnp.arange(pairs, dtype=jnp.int32) // (TOK_DEV * TOP_K)).astype(jnp.int32)
    position = (block * CAP + slot).astype(jnp.int32)
    owner = (jnp.arange(pairs, dtype=jnp.int32) // TOP_K).astype(jnp.int32)
    source = jnp.full((EXPERTS, N_EP * CAP), TOKENS, jnp.int32).at[flat, position].set(owner)
    weights = jnp.zeros((EXPERTS, N_EP * CAP), jnp.float32).at[flat, position].set(route_weights.reshape(-1).astype(jnp.float32))
    padded = jnp.concatenate([normed, jnp.zeros((1, normed.shape[1]), jnp.bfloat16)], axis=0)

    def one_expert(total, inputs):
        rows_idx, row_w, w_gate, w_up, w_down = inputs
        rows = padded[rows_idx]
        gate = jnp.dot(rows, w_gate, preferred_element_type=jnp.float32)
        upper = jnp.dot(rows, w_up, preferred_element_type=jnp.float32)
        hidden = (jax.nn.silu(gate) * upper).astype(jnp.bfloat16)
        result = jnp.dot(hidden, w_down, preferred_element_type=jnp.float32).astype(jnp.bfloat16)
        total = total.at[rows_idx].add(result.astype(jnp.float32) * row_w[:, None])
        return (total, None)
    start = jnp.zeros((TOKENS + 1, normed.shape[1]), jnp.float32)
    total, _ = lax.scan(one_expert, start, (source, weights, gate_weight, up_weight, down_weight))
    return total[:TOKENS].astype(jnp.bfloat16)
```

```python
import functools

import jax
import jax.numpy as jnp
from jax import lax
from jax.experimental import pallas as pl
from jax.experimental.pallas import tpu as pltpu
from jax.sharding import PartitionSpec as P

MESH = pl.DeviceIdType.MESH
COLS = 2


def normalize(rows, norm_gain):
    xf = rows.astype(jnp.float32)
    scale = lax.rsqrt(jnp.mean(xf * xf, axis=-1, keepdims=True) + 1e-06)
    return (xf * scale * norm_gain[None, :]).astype(jnp.bfloat16)


def sparse_form(tokens, norm_gain, expert_ids, route_weights, gate_weight, up_weight, down_weight):
    tok_rows, half = tokens.shape
    width = half * lax.axis_size("tp")
    experts = lax.axis_size("ep")
    top = expert_ids.shape[1]
    capacity = max(2, (3 * tok_rows * top + 2 * experts - 1) // (2 * experts))
    flat = expert_ids.reshape(-1)
    onehot = (flat[:, None] == jnp.arange(experts, dtype=jnp.int32)[None, :]).astype(jnp.int32)
    earlier = jnp.cumsum(onehot, axis=0) - onehot
    slot = jnp.sum(earlier * onehot, axis=-1)
    position = flat * capacity + slot
    owner = jnp.arange(flat.shape[0], dtype=jnp.int32) // top
    w_gate = gate_weight[0]
    w_up = up_weight[0]
    w_down = down_weight[0]
    send = jnp.zeros((experts * capacity, half), jnp.bfloat16).at[position].set(tokens[owner])
    send = send.reshape(experts, capacity, half)
    received = lax.all_to_all(send, "ep", split_axis=0, concat_axis=0, tiled=True)
    sources = received.shape[0]
    count = received.shape[1]
    whole_rows = lax.all_gather(received, "tp", axis=2, tiled=True)
    rows = normalize(whole_rows.reshape(sources * count, width), norm_gain)
    gate = jnp.dot(rows, w_gate, preferred_element_type=jnp.float32)
    upper = jnp.dot(rows, w_up, preferred_element_type=jnp.float32)
    hidden = (jax.nn.silu(gate) * upper).astype(jnp.bfloat16)
    result = jnp.dot(
        lax.all_gather(hidden, "tp", axis=1, tiled=True), w_down, preferred_element_type=jnp.float32
    )
    result = result.astype(jnp.bfloat16).reshape(sources, count, half)
    back = lax.all_to_all(result, "ep", split_axis=0, concat_axis=0, tiled=True)
    picked = back.reshape(experts * capacity, half)[position].astype(jnp.float32)
    picked = picked * route_weights.reshape(-1)[:, None]
    return jnp.sum(picked.reshape(tok_rows, top, half), axis=1).astype(jnp.bfloat16)


def line_kernel(
    length, tok_ref, gain_ref, route_ref, gate_in, up_in, down_in, out_ref,
    raw, x, wt, wg, wu, wd, hid, acc, part, from_low, from_high, fin, outs,
    swap_s, swap_r, loc, own_s, own_r, wy_s, wy_r, wx_s, wx_r, p1_s, p1_r, p2_s, p2_r,
    up_s, up_r, dn_s, dn_r, upt_s, upt_r, dnt_s, dnt_r, ru_s, ru_r, rd_s, rd_r, fin_s, fin_r,
):
    f32 = jnp.float32
    g, ep, c = lax.axis_index("grp"), lax.axis_index("ep"), lax.axis_index("tp")
    z, y = ep // COLS, ep % COLS
    last = length - 1
    mate, across, beside = {"tp": 1 - c}, {"grp": 1 - g}, {"ep": z * COLS + 1 - y}
    above, below = {"ep": ep + COLS}, {"ep": ep - COLS}
    rows, half = raw.shape[1], raw.shape[2]
    piece = rows // 2

    def remote(src, dst, ss, rs, dev):
        return pltpu.make_async_remote_copy(
            src_ref=src, dst_ref=dst, send_sem=ss, recv_sem=rs, device_id=dev, device_id_type=MESH
        )

    barrier = pltpu.get_barrier_semaphore()
    for dev in (mate, across, beside):
        pl.semaphore_signal(barrier, inc=1, device_id=dev, device_id_type=MESH)

    @pl.when(z < last)
    def _():
        pl.semaphore_signal(barrier, inc=1, device_id=above, device_id_type=MESH)

    @pl.when(z > 0)
    def _():
        pl.semaphore_signal(barrier, inc=1, device_id=below, device_id_type=MESH)

    ends = jnp.where(z == 0, 1, 0) + jnp.where(z == last, 1, 0)
    pl.semaphore_wait(barrier, 5 - ends)

    swap = remote(tok_ref.at[1 - c], raw.at[c], swap_s, swap_r, mate)
    swap.start()

    mats = ((gate_in, wg), (up_in, wu), (down_in, wd))
    chunks = []
    for m in range(3):
        quarter = mats[m][0].shape[0] // 4
        for u in range(2):
            chunks.append((m, u, quarter))

    def cut(portion, u, quarter):
        return pl.ds(pl.multiple_of((portion * 2 + u) * quarter, quarter), quarter)

    def send_y(t):
        m, u, q = chunks[t]
        src, dst = mats[m]
        return remote(src.at[cut(g, u, q)], dst.at[1, c, cut(g, u, q)], wy_s.at[t], wy_r.at[t], beside)

    def send_x(t, portion):
        m, u, q = chunks[t]
        buf = mats[m][1].at[1, c, cut(portion, u, q)]
        return remote(buf, buf, wx_s.at[t], wx_r.at[t], across)

    def send_mate(t, portion, half_of, ss, rs):
        m, u, q = chunks[t]
        buf = mats[m][1].at[1, half_of, cut(portion, u, q)]
        return remote(buf, buf, ss.at[t], rs.at[t], mate)

    for t in range(6):
        send_y(t).start()
    own = []
    for m in range(3):
        src, dst = mats[m]
        own.append(remote(src, dst.at[0, c], own_s.at[m], own_r.at[m], mate))
    local = [pltpu.make_async_copy(mats[m][0], mats[m][1].at[0, c], loc.at[m]) for m in range(3)]

    for copy in own + local:
        copy.start()
    wt[z] = route_ref[...]
    swap.wait_recv()
    step = rows // 8

    def norm(i, carry):
        at = pl.ds(pl.multiple_of(i * step, step), step)
        a = tok_ref[c, at].astype(f32)
        b = raw[1 - c, at].astype(f32)
        total = jnp.sum(a * a, axis=-1, keepdims=True) + jnp.sum(b * b, axis=-1, keepdims=True)
        scale = lax.rsqrt(total / (2 * half) + 1e-06)
        x[z, c, at] = (a * scale * gain_ref[c]).astype(x.dtype)
        x[z, 1 - c, at] = (b * scale * gain_ref[1 - c]).astype(x.dtype)
        return carry

    lax.fori_loop(0, 8, norm, 0)

    def rise(b):
        return (
            remote(x.at[b], x.at[b], up_s.at[b], up_r.at[b], above),
            remote(wt.at[b], wt.at[b], upt_s.at[b], upt_r.at[b], above),
        )

    def fall(b):
        return (
            remote(x.at[b], x.at[b], dn_s.at[b], dn_r.at[b], below),
            remote(wt.at[b], wt.at[b], dnt_s.at[b], dnt_r.at[b], below),
        )

    @pl.when(z < last)
    def _():
        for copy in rise(z):
            copy.start()

    @pl.when(z > 0)
    def _():
        for copy in fall(z):
            copy.start()

    def hand_on(k):
        @pl.when(z >= k)
        def _():
            for copy in rise(z - k):
                copy.wait_recv()

            @pl.when(z < last)
            def _():
                for copy in rise(z - k):
                    copy.start()

        @pl.when(z + k <= last)
        def _():
            for copy in fall(z + k):
                copy.wait_recv()

            @pl.when(z > 0)
            def _():
                for copy in fall(z + k):
                    copy.start()

    def got_y(t):
        m, u, q = chunks[t]
        send_y(t).wait_recv()
        send_x(t, g).start()
        send_mate(t, g, c, p1_s, p1_r).start()

    def got_x(t):
        send_x(t, 1 - g).wait_recv()
        send_mate(t, 1 - g, c, p2_s, p2_r).start()

    for t in range(6):
        got_y(t)
        if t >= 1:
            got_x(t - 1)
        if t == 3:
            hand_on(1)
    got_x(5)
    for t in range(6):
        send_mate(t, g, 1 - c, p1_s, p1_r).wait_recv()
        send_mate(t, 1 - g, 1 - c, p2_s, p2_r).wait_recv()
    for m in range(3):
        local[m].wait()
        own[m].wait_recv()

    def experts_on(b):
        columns = wt[b].T
        lane = lax.broadcasted_iota(jnp.int32, columns.shape, 1)
        for s in range(2):
            expert = z * COLS + (y if s == 0 else 1 - y)
            weight = jnp.sum(jnp.where(lane == expert, columns, 0.0), axis=1, keepdims=True)
            for h in range(2):
                both = []
                for w in (wg, wu):
                    both.append(
                        jnp.dot(x[b, 0], w[s, h, :half], preferred_element_type=f32)
                        + jnp.dot(x[b, 1], w[s, h, half:], preferred_element_type=f32)
                    )
                gate, upper = both
                silu = gate * (0.5 * (1.0 + jnp.tanh(0.5 * gate)))
                wide = gate.shape[1]
                hid[:, h * wide:(h + 1) * wide] = (silu * upper).astype(hid.dtype)
            for f in range(2):
                got = jnp.dot(hid[...], wd[s, f], preferred_element_type=f32)
                got = got.astype(jnp.bfloat16).astype(f32) * weight
                if s == 0:
                    acc[f] = got
                else:
                    got = acc[f] + got
                    acc[f] = got
                    part[b, f] = got.astype(part.dtype)

    def place(j):
        return (1 - c if j < 2 else c), pl.ds((j % 2) * piece, piece)

    def sum_up(b, j):
        f, at = place(j)
        return remote(part.at[b, f, at], from_low.at[b, f, at], ru_s.at[b, j], ru_r.at[b, j], above)

    def sum_down(b, j):
        f, at = place(j)
        return remote(part.at[b, f, at], from_high.at[b, f, at], rd_s.at[b, j], rd_r.at[b, j], below)

    def stage(k, carry):
        @pl.when(k > 1)
        def _():
            hand_on(k)

        def one(i, inner):
            b = jnp.where(k > last, z, jnp.where(i == 0, z - k, z + k))

            @pl.when((b >= 0) & (b <= last) & ((k <= last) | (i == 0)))
            def _():
                experts_on(b)
            return inner

        lax.fori_loop(0, 2, one, 0)

        for j in range(4):
            f, at = place(j)

            @pl.when((z < k) & (k <= last))
            def _():
                @pl.when(z > 0)
                def _():
                    sum_up(k, j).wait_recv()
                    part[k, f, at] = (part[k, f, at].astype(f32) + from_low[k, f, at].astype(f32)).astype(part.dtype)
                sum_up(k, j).start()

            low = last - k

            @pl.when((z > low) & (k <= last))
            def _():
                @pl.when(z < last)
                def _():
                    sum_down(low, j).wait_recv()
                    part[low, f, at] = (
                        part[low, f, at].astype(f32) + from_high[low, f, at].astype(f32)
                    ).astype(part.dtype)
                sum_down(low, j).start()
        return carry

    lax.fori_loop(1, length + 1, stage, 0)

    def give(r):
        at = pl.ds(r * piece, piece)
        return remote(fin.at[at], outs.at[c, at], fin_s.at[r], fin_r.at[r], mate)

    for j in range(4):
        f, at = place(j)

        @pl.when(z > 0)
        def _():
            sum_up(z, j).wait_recv()
            acc[f, at] = acc[f, at] + from_low[z, f, at].astype(f32)

        @pl.when(z < last)
        def _():
            sum_down(z, j).wait_recv()
            acc[f, at] = acc[f, at] + from_high[z, f, at].astype(f32)

        if j < 2:
            fin[at] = acc[f, at].astype(fin.dtype)
            give(j).start()
        else:
            out_ref[c, at] = acc[f, at].astype(out_ref.dtype)
    for r in range(2):
        at = pl.ds(r * piece, piece)
        give(r).wait_recv()
        out_ref[1 - c, at] = outs[1 - c, at]

    swap.wait_send()
    for copy in own:
        copy.wait_send()
    for t in range(6):
        send_y(t).wait_send()
        send_x(t, g).wait_send()
        send_mate(t, g, c, p1_s, p1_r).wait_send()
        send_mate(t, 1 - g, c, p2_s, p2_r).wait_send()
    for r in range(2):
        give(r).wait_send()
    for b in range(length):
        @pl.when((z >= b) & (z < last))
        def _():
            for copy in rise(b):
                copy.wait_send()

        @pl.when((z <= b) & (z > 0))
        def _():
            for copy in fall(b):
                copy.wait_send()

        @pl.when(z < b)
        def _():
            for j in range(4):
                sum_up(b, j).wait_send()

        @pl.when(z > b)
        def _():
            for j in range(4):
                sum_down(b, j).wait_send()


def line_form(tokens, norm_gain, expert_ids, route_weights, gate_weight, up_weight, down_weight):
    tok_rows, half = tokens.shape
    experts = lax.axis_size("ep")
    length = experts // COLS
    rows = tok_rows // 2
    mine = lax.axis_index("tp")
    bf16, f32 = jnp.bfloat16, jnp.float32
    chosen = expert_ids[None] == jnp.arange(experts, dtype=jnp.int32)[:, None, None]
    route = jnp.sum(jnp.where(chosen, route_weights[None], 0.0), axis=-1)
    route = lax.dynamic_slice_in_dim(route, mine * rows, rows, axis=1)
    gate, up, down = gate_weight[0], up_weight[0], down_weight[0]
    dma, vmem = pltpu.SemaphoreType.DMA, pltpu.VMEM
    block = (length, 2, rows, half)
    sems = []
    for shape in (
        (1,), (3,), (6,), (6,), (6,), (6,), (length,), (length,), (length,), (length,), (length, 4), (length, 4), (2,)
    ):
        sems += [dma(shape), dma(shape)]
    sems = [dma, dma, dma((3,))] + sems[2:]
    out = pl.pallas_call(
        functools.partial(line_kernel, length),
        out_shape=jax.ShapeDtypeStruct((2, rows, half), bf16),
        in_specs=[pl.BlockSpec(memory_space=vmem)] * 3 + [pl.BlockSpec(memory_space=pl.ANY)] * 3,
        out_specs=pl.BlockSpec(memory_space=vmem),
        scratch_shapes=[
            vmem((2, rows, half), bf16),
            vmem(block, bf16),
            vmem((length, experts, rows), f32),
            vmem((2, 2) + gate.shape, bf16),
            vmem((2, 2) + up.shape, bf16),
            vmem((2, 2) + down.shape, bf16),
            vmem((rows, 2 * gate.shape[1]), bf16),
            vmem((2, rows, half), f32),
            vmem(block, bf16),
            vmem(block, bf16),
            vmem(block, bf16),
            vmem((rows, half), bf16),
            vmem((2, rows, half), bf16),
        ]
        + sems,
        compiler_params=pltpu.CompilerParams(
            collective_id=0, has_side_effects=True, vmem_limit_bytes=60 * 1024 * 1024
        ),
    )(tokens.reshape(2, rows, half), norm_gain.reshape(2, 1, half), route, gate, up, down)
    return out.reshape(tok_rows, half)


def solution(mesh):
    in_specs = (
        P(("grp", "ep"), "tp"),
        P(),
        P(("grp", "ep"), None),
        P(("grp", "ep"), None),
        P("ep", None, "tp"),
        P("ep", None, "tp"),
        P("ep", None, "tp"),
    )
    out_specs = P(("grp", "ep"), "tp")
    shape = mesh.shape

    def on_device(tokens, norm_gain, expert_ids, *rest):
        dense = shape["ep"] <= 4 * expert_ids.shape[1] and shape["ep"] % COLS == 0 and shape["ep"] > COLS
        form = line_form if dense and shape["grp"] == 2 and shape["tp"] == 2 else sparse_form
        return form(tokens, norm_gain, expert_ids, *rest)

    return jax.shard_map(
        on_device, mesh=mesh, in_specs=in_specs, out_specs=out_specs, check_vma=False
    )
```

```python
import functools

import jax
import jax.numpy as jnp
from jax import lax
from jax.experimental import pallas as pl
from jax.experimental.pallas import tpu as pltpu
from jax.sharding import PartitionSpec as P

MESH = pl.DeviceIdType.MESH
COLS = 2
PARTS = 8
CUTS = 4


def normalize(rows, norm_gain):
    xf = rows.astype(jnp.float32)
    scale = lax.rsqrt(jnp.mean(xf * xf, axis=-1, keepdims=True) + 1e-06)
    return (xf * scale * norm_gain[None, :]).astype(jnp.bfloat16)


def sparse_form(tokens, norm_gain, expert_ids, route_weights, gate_weight, up_weight, down_weight):
    tok_rows, half = tokens.shape
    width = half * lax.axis_size("tp")
    experts = lax.axis_size("ep")
    top = expert_ids.shape[1]
    capacity = max(2, (3 * tok_rows * top + 2 * experts - 1) // (2 * experts))
    flat = expert_ids.reshape(-1)
    onehot = (flat[:, None] == jnp.arange(experts, dtype=jnp.int32)[None, :]).astype(jnp.int32)
    earlier = jnp.cumsum(onehot, axis=0) - onehot
    slot = jnp.sum(earlier * onehot, axis=-1)
    position = flat * capacity + slot
    owner = jnp.arange(flat.shape[0], dtype=jnp.int32) // top
    w_gate = gate_weight[0]
    w_up = up_weight[0]
    w_down = down_weight[0]
    send = jnp.zeros((experts * capacity, half), jnp.bfloat16).at[position].set(tokens[owner])
    send = send.reshape(experts, capacity, half)
    received = lax.all_to_all(send, "ep", split_axis=0, concat_axis=0, tiled=True)
    sources = received.shape[0]
    count = received.shape[1]
    whole_rows = lax.all_gather(received, "tp", axis=2, tiled=True)
    rows = normalize(whole_rows.reshape(sources * count, width), norm_gain)
    gate = jnp.dot(rows, w_gate, preferred_element_type=jnp.float32)
    upper = jnp.dot(rows, w_up, preferred_element_type=jnp.float32)
    hidden = (jax.nn.silu(gate) * upper).astype(jnp.bfloat16)
    result = jnp.dot(
        lax.all_gather(hidden, "tp", axis=1, tiled=True), w_down, preferred_element_type=jnp.float32
    )
    result = result.astype(jnp.bfloat16).reshape(sources, count, half)
    back = lax.all_to_all(result, "ep", split_axis=0, concat_axis=0, tiled=True)
    picked = back.reshape(experts * capacity, half)[position].astype(jnp.float32)
    picked = picked * route_weights.reshape(-1)[:, None]
    return jnp.sum(picked.reshape(tok_rows, top, half), axis=1).astype(jnp.bfloat16)


def line_kernel(
    length, tok_ref, gain_ref, route_ref, gate_in, up_in, down_in, out_ref,
    raw, x, wt, wg, wu, wd, hid, acc, part, from_low, from_high, fin, outs,
    swap_s, swap_r, loc, own_s, own_r, wy_s, wy_r, wx_s, wx_r, p1_s, p1_r, p2_s, p2_r,
    up_s, up_r, dn_s, dn_r, upt_s, upt_r, dnt_s, dnt_r, ru_s, ru_r, rd_s, rd_r, fin_s, fin_r,
):
    f32 = jnp.float32
    g, ep, c = lax.axis_index("grp"), lax.axis_index("ep"), lax.axis_index("tp")
    z, y = ep // COLS, ep % COLS
    last = length - 1
    mate, across, beside = {"tp": 1 - c}, {"grp": 1 - g}, {"ep": z * COLS + 1 - y}
    above, below = {"ep": ep + COLS}, {"ep": ep - COLS}
    rows, half = raw.shape[1], raw.shape[2]
    piece = rows // (PARTS // 2)

    def remote(src, dst, ss, rs, dev):
        return pltpu.make_async_remote_copy(
            src_ref=src, dst_ref=dst, send_sem=ss, recv_sem=rs, device_id=dev, device_id_type=MESH
        )

    barrier = pltpu.get_barrier_semaphore()
    for dev in (mate, across, beside):
        pl.semaphore_signal(barrier, inc=1, device_id=dev, device_id_type=MESH)

    @pl.when(z < last)
    def _():
        pl.semaphore_signal(barrier, inc=1, device_id=above, device_id_type=MESH)

    @pl.when(z > 0)
    def _():
        pl.semaphore_signal(barrier, inc=1, device_id=below, device_id_type=MESH)

    ends = jnp.where(z == 0, 1, 0) + jnp.where(z == last, 1, 0)
    pl.semaphore_wait(barrier, 5 - ends)

    swap = remote(tok_ref.at[1 - c], raw.at[c], swap_s, swap_r, mate)
    swap.start()

    mats = ((gate_in, wg), (up_in, wu), (down_in, wd))
    chunks = []
    for m in range(3):
        size = mats[m][0].shape[0] // (2 * CUTS)
        for u in range(CUTS):
            chunks.append((m, u, size))
    amount = len(chunks)

    def cut(portion, u, size):
        return pl.ds(pl.multiple_of((portion * CUTS + u) * size, size), size)

    def send_y(t):
        m, u, q = chunks[t]
        src, dst = mats[m]
        return remote(src.at[cut(g, u, q)], dst.at[1, c, cut(g, u, q)], wy_s.at[t], wy_r.at[t], beside)

    def send_x(t, portion):
        m, u, q = chunks[t]
        buf = mats[m][1].at[1, c, cut(portion, u, q)]
        return remote(buf, buf, wx_s.at[t], wx_r.at[t], across)

    def send_mate(t, portion, half_of, ss, rs):
        m, u, q = chunks[t]
        buf = mats[m][1].at[1, half_of, cut(portion, u, q)]
        return remote(buf, buf, ss.at[t], rs.at[t], mate)

    for t in range(amount):
        send_y(t).start()
    own = []
    for m in range(3):
        src, dst = mats[m]
        own.append(remote(src, dst.at[0, c], own_s.at[m], own_r.at[m], mate))
    local = [pltpu.make_async_copy(mats[m][0], mats[m][1].at[0, c], loc.at[m]) for m in range(3)]

    for copy in own + local:
        copy.start()
    wt[z] = route_ref[...]
    swap.wait_recv()
    step = rows // 8

    def norm(i, carry):
        at = pl.ds(pl.multiple_of(i * step, step), step)
        a = tok_ref[c, at].astype(f32)
        b = raw[1 - c, at].astype(f32)
        total = jnp.sum(a * a, axis=-1, keepdims=True) + jnp.sum(b * b, axis=-1, keepdims=True)
        scale = lax.rsqrt(total / (2 * half) + 1e-06)
        x[z, c, at] = (a * scale * gain_ref[c]).astype(x.dtype)
        x[z, 1 - c, at] = (b * scale * gain_ref[1 - c]).astype(x.dtype)
        return carry

    lax.fori_loop(0, 8, norm, 0)

    def rise(b):
        return (
            remote(x.at[b], x.at[b], up_s.at[b], up_r.at[b], above),
            remote(wt.at[b], wt.at[b], upt_s.at[b], upt_r.at[b], above),
        )

    def fall(b):
        return (
            remote(x.at[b], x.at[b], dn_s.at[b], dn_r.at[b], below),
            remote(wt.at[b], wt.at[b], dnt_s.at[b], dnt_r.at[b], below),
        )

    @pl.when(z < last)
    def _():
        for copy in rise(z):
            copy.start()

    @pl.when(z > 0)
    def _():
        for copy in fall(z):
            copy.start()

    def hand_on(k):
        @pl.when(z >= k)
        def _():
            for copy in rise(z - k):
                copy.wait_recv()

            @pl.when(z < last)
            def _():
                for copy in rise(z - k):
                    copy.start()

        @pl.when(z + k <= last)
        def _():
            for copy in fall(z + k):
                copy.wait_recv()

            @pl.when(z > 0)
            def _():
                for copy in fall(z + k):
                    copy.start()

    def got_y(t):
        m, u, q = chunks[t]
        send_y(t).wait_recv()
        send_x(t, g).start()
        send_mate(t, g, c, p1_s, p1_r).start()

    def got_x(t):
        send_x(t, 1 - g).wait_recv()
        send_mate(t, 1 - g, c, p2_s, p2_r).start()

    for t in range(amount):
        got_y(t)
        if t >= 1:
            got_x(t - 1)
        if t == 3 * amount // 4 - 1:
            hand_on(1)
    got_x(amount - 1)
    for t in range(amount):
        send_mate(t, g, 1 - c, p1_s, p1_r).wait_recv()
        send_mate(t, 1 - g, 1 - c, p2_s, p2_r).wait_recv()
    for m in range(3):
        local[m].wait()
        own[m].wait_recv()

    def experts_on(b):
        columns = wt[b].T
        lane = lax.broadcasted_iota(jnp.int32, columns.shape, 1)
        for s in range(2):
            expert = z * COLS + (y if s == 0 else 1 - y)
            weight = jnp.sum(jnp.where(lane == expert, columns, 0.0), axis=1, keepdims=True)
            for h in range(2):
                both = []
                for w in (wg, wu):
                    both.append(
                        jnp.dot(x[b, 0], w[s, h, :half], preferred_element_type=f32)
                        + jnp.dot(x[b, 1], w[s, h, half:], preferred_element_type=f32)
                    )
                gate, upper = both
                silu = gate * (0.5 * (1.0 + jnp.tanh(0.5 * gate)))
                wide = gate.shape[1]
                hid[:, h * wide:(h + 1) * wide] = (silu * upper).astype(hid.dtype)
            for f in range(2):
                got = jnp.dot(hid[...], wd[s, f], preferred_element_type=f32)
                got = got.astype(jnp.bfloat16).astype(f32) * weight
                if s == 0:
                    acc[f] = got
                else:
                    got = acc[f] + got
                    acc[f] = got
                    part[b, f] = got.astype(part.dtype)

    def place(j):
        return (1 - c if j < PARTS // 2 else c), pl.ds((j % (PARTS // 2)) * piece, piece)

    def sum_up(b, j):
        f, at = place(j)
        return remote(part.at[b, f, at], from_low.at[b, f, at], ru_s.at[b, j], ru_r.at[b, j], above)

    def sum_down(b, j):
        f, at = place(j)
        return remote(part.at[b, f, at], from_high.at[b, f, at], rd_s.at[b, j], rd_r.at[b, j], below)

    def wave_up(b, j, side):
        f, at = place(j)

        @pl.when(side & (z < b) & (b <= last))
        def _():
            @pl.when(z > 0)
            def _():
                sum_up(b, j).wait_recv()
                part[b, f, at] = (part[b, f, at].astype(f32) + from_low[b, f, at].astype(f32)).astype(part.dtype)
            sum_up(b, j).start()

    def wave_down(b, j, side):
        f, at = place(j)

        @pl.when(side & (z > b) & (b >= 0))
        def _():
            @pl.when(z < last)
            def _():
                sum_down(b, j).wait_recv()
                part[b, f, at] = (part[b, f, at].astype(f32) + from_high[b, f, at].astype(f32)).astype(part.dtype)
            sum_down(b, j).start()

    def stage(k, carry):
        @pl.when(k > 1)
        def _():
            hand_on(k)

        def one(i, inner):
            b = jnp.where(k > last, z, jnp.where(i == 0, z - k, z + k))

            @pl.when((b >= 0) & (b <= last) & ((k <= last) | (i == 0)))
            def _():
                experts_on(b)
            return inner

        lax.fori_loop(0, 2, one, 0)

        for j in range(PARTS + 1):
            if j < PARTS:
                wave_up(k, j, z < length // 2)
                wave_down(last - k, j, z >= length // 2)
            if j > 0:
                wave_down(last - k, j - 1, z < length // 2)
                wave_up(k, j - 1, z >= length // 2)
        return carry

    lax.fori_loop(1, length + 1, stage, 0)

    def give(r):
        at = pl.ds(r * piece, piece)
        return remote(fin.at[at], outs.at[c, at], fin_s.at[r], fin_r.at[r], mate)

    for j in range(PARTS):
        f, at = place(j)

        @pl.when(z > 0)
        def _():
            sum_up(z, j).wait_recv()
            acc[f, at] = acc[f, at] + from_low[z, f, at].astype(f32)

        @pl.when(z < last)
        def _():
            sum_down(z, j).wait_recv()
            acc[f, at] = acc[f, at] + from_high[z, f, at].astype(f32)

        if j < PARTS // 2:
            fin[at] = acc[f, at].astype(fin.dtype)
            give(j).start()
        else:
            out_ref[c, at] = acc[f, at].astype(out_ref.dtype)
    for r in range(PARTS // 2):
        at = pl.ds(r * piece, piece)
        give(r).wait_recv()
        out_ref[1 - c, at] = outs[1 - c, at]

    swap.wait_send()
    for copy in own:
        copy.wait_send()
    for t in range(amount):
        send_y(t).wait_send()
        send_x(t, g).wait_send()
        send_mate(t, g, c, p1_s, p1_r).wait_send()
        send_mate(t, 1 - g, c, p2_s, p2_r).wait_send()
    for r in range(PARTS // 2):
        give(r).wait_send()
    for b in range(length):
        @pl.when((z >= b) & (z < last))
        def _():
            for copy in rise(b):
                copy.wait_send()

        @pl.when((z <= b) & (z > 0))
        def _():
            for copy in fall(b):
                copy.wait_send()

        @pl.when(z < b)
        def _():
            for j in range(PARTS):
                sum_up(b, j).wait_send()

        @pl.when(z > b)
        def _():
            for j in range(PARTS):
                sum_down(b, j).wait_send()


def line_form(tokens, norm_gain, expert_ids, route_weights, gate_weight, up_weight, down_weight):
    tok_rows, half = tokens.shape
    experts = lax.axis_size("ep")
    length = experts // COLS
    rows = tok_rows // 2
    mine = lax.axis_index("tp")
    bf16, f32 = jnp.bfloat16, jnp.float32
    chosen = expert_ids[None] == jnp.arange(experts, dtype=jnp.int32)[:, None, None]
    route = jnp.sum(jnp.where(chosen, route_weights[None], 0.0), axis=-1)
    route = lax.dynamic_slice_in_dim(route, mine * rows, rows, axis=1)
    gate, up, down = gate_weight[0], up_weight[0], down_weight[0]
    dma, vmem = pltpu.SemaphoreType.DMA, pltpu.VMEM
    block = (length, 2, rows, half)
    cuts, sums = (3 * CUTS,), (length, PARTS)
    sems = []
    for shape in (
        (1,), (3,), cuts, cuts, cuts, cuts, (length,), (length,), (length,), (length,), sums, sums, (PARTS // 2,)
    ):
        sems += [dma(shape), dma(shape)]
    sems = [dma, dma, dma((3,))] + sems[2:]
    out = pl.pallas_call(
        functools.partial(line_kernel, length),
        out_shape=jax.ShapeDtypeStruct((2, rows, half), bf16),
        in_specs=[pl.BlockSpec(memory_space=vmem)] * 3 + [pl.BlockSpec(memory_space=pl.ANY)] * 3,
        out_specs=pl.BlockSpec(memory_space=vmem),
        scratch_shapes=[
            vmem((2, rows, half), bf16),
            vmem(block, bf16),
            vmem((length, experts, rows), f32),
            vmem((2, 2) + gate.shape, bf16),
            vmem((2, 2) + up.shape, bf16),
            vmem((2, 2) + down.shape, bf16),
            vmem((rows, 2 * gate.shape[1]), bf16),
            vmem((2, rows, half), f32),
            vmem(block, bf16),
            vmem(block, bf16),
            vmem(block, bf16),
            vmem((rows, half), bf16),
            vmem((2, rows, half), bf16),
        ]
        + sems,
        compiler_params=pltpu.CompilerParams(
            collective_id=0, has_side_effects=True, vmem_limit_bytes=60 * 1024 * 1024
        ),
    )(tokens.reshape(2, rows, half), norm_gain.reshape(2, 1, half), route, gate, up, down)
    return out.reshape(tok_rows, half)


def solution(mesh):
    in_specs = (
        P(("grp", "ep"), "tp"),
        P(),
        P(("grp", "ep"), None),
        P(("grp", "ep"), None),
        P("ep", None, "tp"),
        P("ep", None, "tp"),
        P("ep", None, "tp"),
    )
    out_specs = P(("grp", "ep"), "tp")
    shape = mesh.shape

    def on_device(tokens, norm_gain, expert_ids, *rest):
        dense = shape["ep"] <= 4 * expert_ids.shape[1] and shape["ep"] % COLS == 0 and shape["ep"] > COLS
        form = line_form if dense and shape["grp"] == 2 and shape["tp"] == 2 else sparse_form
        return form(tokens, norm_gain, expert_ids, *rest)

    return jax.shard_map(
        on_device, mesh=mesh, in_specs=in_specs, out_specs=out_specs, check_vma=False
    )
```
